32 devices in a mesh: kv: 8 (over z, y), tp: 4 (over x, core).
Axes of the slice: x: 2, y: 2, z: 4, core: 2. Of those that a mesh axis runs over, the one named last changes fastest.
Arguments:
- tokens: bfloat16 [5120, 4096], P('kv'), may hold values from -48 to 48
- query_weight: bfloat16 [4096, 2048], P(None, 'tp'), may hold values from -0.09375 to 0.09375
- key_weight: bfloat16 [4096, 512], P(None, 'tp'), may hold values from -0.09375 to 0.09375
- value_weight: bfloat16 [4096, 512], P(None, 'tp'), may hold values from -0.09375 to 0.09375
- gate_weight: bfloat16 [4096, 64], replicated, may hold values from -0.09375 to 0.09375
- summary_pos: bfloat16 [32, 64], replicated, may hold values from -6 to 6
- key_mixing: bfloat16 [32, 8], replicated, may hold values from -1 to 1
- value_mixing: bfloat16 [32, 8], replicated, may hold values from -1 to 1
- out_weight: bfloat16 [2048, 4096], P('tp'), may hold values from -0.125 to 0.125
- chosen: int32 [80, 8, 16], P('kv', 'tp'), may hold values from 0 to 79, as said below
Outputs:
- mixed: bfloat16 [5120, 4096], P(('kv', 'tp'))
The draws below stay inside these ranges and needn't reach their ends.
Inputs may be any that keep to these rules, and one draw needn't show every extreme that they name: `chosen`: entry [b, g, 0] is b itself; every entry is at most b. For the query blocks of one index of kv, one key head and any OTHER index of kv, at most 2 distinct blocks of that index's 64-position blocks are named, and exactly 2 of the index just before. Entries may repeat.
All inputs are finite; a program needn't handle non-finite values.
Results may differ from the reference program's by a relative error of at most 0.013.
The reference program's roundings to bfloat16 on the way count: a program that leaves them out, or rounds other values in their place, can miss the bound.
Values may be sent and summed in bfloat16 or wider, within the bound.
A program may use at most 192 MiB of HBM per device.

```python
import jax
import jax.numpy as jnp
from jax import lax

D = 4096
HEADS = 32
KV_HEADS = 8
HD = 64
CMP = 32
SB = 64
N_SEL = 16
CAP = 2
TOK_DEV = 640
TOKENS = 5120
N_TP = 4


def draw_tokens(key, part):
    base = jax.random.normal(key, (TOKENS, D), jnp.float32)
    return jnp.clip(base, -6.0, 6.0).astype(jnp.bfloat16)


def draw_chosen(key, part):
    per_device = TOK_DEV // SB
    block_total = TOKENS // SB
    device_total = block_total // per_device
    grid_shape = (block_total, KV_HEADS, N_SEL)
    column_shape = (block_total, KV_HEADS, 1)
    streams = jax.random.split(key, 8)
    query_block = jnp.arange(block_total, dtype=jnp.int32)[:, None, None]
    device_of = query_block // per_device
    head_ids = jnp.arange(KV_HEADS, dtype=jnp.int32)[None, :, None]
    first_pick = jax.random.randint(streams[0], (device_total, KV_HEADS, device_total), 0, per_device)
    pick_step = jax.random.randint(streams[1], (device_total, KV_HEADS, device_total), 1, per_device)
    popular = jax.random.randint(streams[2], (4,), 0, device_total)
    use_popular = jax.random.randint(streams[3], grid_shape, 0, 2)
    popular_pick = popular[jax.random.randint(streams[4], grid_shape, 0, 4)]
    drawn_pick = jax.random.randint(streams[5], grid_shape, 0, device_of + 1)
    source = jnp.where((use_popular == 1) & (popular_pick <= device_of), popular_pick, drawn_pick)
    which = jax.random.randint(streams[6], grid_shape, 0, CAP)
    candidate = (first_pick[device_of, head_ids, source] + which * pick_step[device_of, head_ids, source]) % per_device
    at_home = jax.random.randint(streams[7], grid_shape, device_of * per_device, query_block + 1)
    picks = jnp.where(source == device_of, at_home, source * per_device + candidate)
    before = jnp.maximum(device_of - 1, 0)
    half_away = jnp.maximum(device_of - device_total // 2, 0)
    first_before = first_pick[device_of, head_ids, before]
    own_block = jnp.broadcast_to(query_block, column_shape)
    slot_one = jnp.where(device_of >= 1, before * per_device + first_before, own_block)
    slot_two = jnp.where(device_of >= device_total // 2, half_away * per_device + first_pick[device_of, head_ids, half_away], own_block)
    slot_three = jnp.where(device_of >= 1, before * per_device + (first_before + pick_step[device_of, head_ids, before]) % per_device, own_block)
    return jnp.concatenate([own_block, jnp.broadcast_to(slot_one, column_shape), jnp.broadcast_to(slot_two, column_shape), jnp.broadcast_to(slot_three, column_shape), picks[:, :, 4:]], axis=2).astype(jnp.int32)


def shard_levels(stream_key, shape, pieces, smallest, high):
    def one(position, shards_of):
        draws = jax.random.uniform(jax.random.fold_in(jax.random.fold_in(stream_key, 6), position), (shards_of,), jnp.float32, smallest / len(pieces), high / len(pieces))
        return jnp.repeat(jnp.exp(draws), shape[position] // shards_of).reshape((-1,) + (1,) * (len(shape) - position - 1))

    gain = one(*pieces[0])
    for cut in pieces[1:]:
        gain = gain * one(*cut)
    return gain


def bell_draw(rng, extent, spread, most, cuts=(), kind=jnp.bfloat16):
    result = jax.random.normal(rng, extent, jnp.float32) * spread
    if len(cuts) > 0:
        result = shard_levels(rng, extent, cuts, -0.22, 0.18) * result
    return jnp.clip(result, min=-most, max=most).astype(kind)


def setup_inputs(seed: int = 0) -> dict:
    arg_keys = jax.random.split(jax.random.key(seed), 11)
    return {
        "tokens": draw_tokens(jax.random.fold_in(arg_keys[10], 71), 0),
        "query_weight": bell_draw(arg_keys[1], (D, HEADS * HD), D ** -0.5, 0.09375, ((1, 4),)),
        "key_weight": bell_draw(arg_keys[2], (D, KV_HEADS * HD), D ** -0.5, 0.09375, ((1, 4),)),
        "value_weight": bell_draw(arg_keys[3], (D, KV_HEADS * HD), D ** -0.5, 0.09375, ((1, 4),)),
        "gate_weight": bell_draw(arg_keys[4], (D, 2 * HEADS), D ** -0.5, 0.09375),
        "summary_pos": bell_draw(arg_keys[5], (CMP, HD), 1.0, 6.0),
        "key_mixing": bell_draw(arg_keys[6], (CMP, KV_HEADS), CMP ** -0.5, 1.0),
        "value_mixing": bell_draw(arg_keys[7], (CMP, KV_HEADS), CMP ** -0.5, 1.0),
        "out_weight": bell_draw(arg_keys[8], (HEADS * HD, D), (HEADS * HD) ** -0.5, 0.125, ((0, 4),)),
        "chosen": draw_chosen(jax.random.fold_in(arg_keys[10], 71), 0),
    }


floor_score = -1e30


def masked_weights(scores, visible):
    probs = jax.nn.softmax(jnp.where(visible, scores, floor_score), axis=-1)
    return jnp.where(jnp.any(visible, axis=-1, keepdims=True), probs, 0.0)


def first_named(picked_ids):
    slot_count = picked_ids.shape[-1]
    repeated = picked_ids[..., :, None] == picked_ids[..., None, :]
    earlier = jnp.arange(slot_count)[None, :] < jnp.arange(slot_count)[:, None]
    return jnp.logical_not(jnp.any(repeated & earlier, axis=-1))


def summarize(source, offsets, mixing):
    span_count = source.shape[0] // CMP
    windows = source.astype(jnp.float32).reshape(span_count, CMP, source.shape[1], HD)
    windows = windows + offsets.astype(jnp.float32)[None, :, None, :]
    return jnp.einsum('njgd,jg->ngd', windows, mixing.astype(jnp.float32),
                      precision=lax.Precision.HIGHEST).astype(jnp.bfloat16)


def reference(tokens, query_weight, key_weight, value_weight, gate_weight, summary_pos, key_mixing,
              value_mixing, out_weight, chosen):
    length = tokens.shape[0]
    group_size = HEADS // KV_HEADS
    score_scale = HD ** -0.5
    queries = jnp.dot(tokens, query_weight, preferred_element_type=jnp.float32).astype(jnp.bfloat16)
    key_rows = jnp.dot(tokens, key_weight, preferred_element_type=jnp.float32).astype(jnp.bfloat16)
    key_rows = key_rows.reshape(length, KV_HEADS, HD)
    value_rows = jnp.dot(tokens, value_weight, preferred_element_type=jnp.float32).astype(jnp.bfloat16)
    value_rows = value_rows.reshape(length, KV_HEADS, HD)
    gate_vals = jax.nn.sigmoid(jnp.dot(tokens, gate_weight, preferred_element_type=jnp.float32))
    gate_vals = gate_vals.reshape(length // SB, SB, KV_HEADS, group_size, 2)
    key_summary = summarize(key_rows, summary_pos, key_mixing).astype(jnp.float32)
    value_summary = summarize(value_rows, summary_pos, value_mixing).astype(jnp.float32)
    span_ends = jnp.arange(length // CMP, dtype=jnp.int32) * CMP + (CMP - 1)
    block_table = jnp.concatenate([key_rows, value_rows], axis=-1).reshape(length // SB, SB, KV_HEADS, 2 * HD)
    head_ids = jnp.arange(KV_HEADS, dtype=jnp.int32)[:, None]
    unique_all = first_named(chosen)

    def one_block(inputs):
        query_blk, gate_blk, picked_ids, unique, offset = inputs
        query_pos = offset + jnp.arange(SB, dtype=jnp.int32)
        query_f = query_blk.astype(jnp.float32).reshape(SB, KV_HEADS, group_size, HD)
        summary_scores = jnp.einsum('qgrd,ngd->grqn', query_f, key_summary) * score_scale
        summary_probs = masked_weights(summary_scores, (span_ends[None, :] <= query_pos[:, None])[None, None])
        summary_probs = lax.optimization_barrier(summary_probs.astype(jnp.bfloat16)).astype(jnp.float32)
        summary_out = jnp.einsum('grqn,ngd->qgrd', summary_probs, value_summary)
        picked = block_table[picked_ids, :, head_ids, :]
        picked = picked.reshape(KV_HEADS, N_SEL * SB, 2 * HD).astype(jnp.float32)
        key_pos = (picked_ids[:, :, None] * SB + jnp.arange(SB, dtype=jnp.int32)).reshape(KV_HEADS, N_SEL * SB)
        counted = jnp.broadcast_to(unique[:, :, None], (KV_HEADS, N_SEL, SB)).reshape(KV_HEADS, N_SEL * SB)
        visible = counted[:, None, :] & (key_pos[:, None, :] <= query_pos[None, :, None])
        chosen_scores = jnp.einsum('qgrd,gmd->grqm', query_f, picked[..., :HD]) * score_scale
        chosen_probs = masked_weights(chosen_scores, visible[:, None])
        chosen_probs = lax.optimization_barrier(chosen_probs.astype(jnp.bfloat16)).astype(jnp.float32)
        chosen_out = jnp.einsum('grqm,gmd->qgrd', chosen_probs, picked[..., HD:])
        blended = gate_blk[..., 0:1] * summary_out + gate_blk[..., 1:2] * chosen_out
        return blended.reshape(SB, HEADS * HD).astype(jnp.bfloat16)

    offsets = jnp.arange(length // SB, dtype=jnp.int32) * SB
    attention = lax.map(one_block, (queries.reshape(length // SB, SB, HEADS * HD), gate_vals, chosen,
                                    unique_all, offsets)).reshape(length, HEADS * HD)
    width = HEADS * HD // N_TP
    summed = jnp.zeros((length, D), jnp.float32)
    for head_part in range(N_TP):
        partial_value = jnp.dot(attention[:, head_part * width:(head_part + 1) * width],
                          out_weight[head_part * width:(head_part + 1) * width],
                          preferred_element_type=jnp.float32).astype(jnp.bfloat16)
        summed = summed + lax.optimization_barrier(partial_value).astype(jnp.float32)
    return summed.astype(jnp.bfloat16)
```

```python
import functools

import jax
import jax.numpy as jnp
from jax import lax
from jax.experimental import pallas as pl
from jax.experimental.pallas import tpu as pltpu
from jax.sharding import PartitionSpec as P

HD = 64
CMP = 32
SB = 64
N_SEL = 16
LANES = 128
LOW = -1e30
F32 = jnp.float32
BF16 = jnp.bfloat16
MESH = pl.DeviceIdType.MESH
VMEM_LIMIT = 64_000_000


def first_named(picked_ids):
    slot_count = picked_ids.shape[-1]
    repeated = picked_ids[..., :, None] == picked_ids[..., None, :]
    earlier = jnp.arange(slot_count)[None, :] < jnp.arange(slot_count)[:, None]
    return jnp.logical_not(jnp.any(repeated & earlier, axis=-1))


def project_kernel(
    n, G, R, nb, kc, pad,
    tok_hbm, qw_hbm, kw_hbm, vw_hbm, gw_hbm, req_ref, mix_ref, pos_ref,
    qp_ref, gate_ref, tab_ref, sum_ref,
    tok, qw, kvw, gw, acc, gacc, tf, req_in, send, sum_send,
    sem_tok, sem_kw, sem_vw, sem_qw, sem_gw,
    req_s, req_r, blk_s, blk_r, sum_s, sum_r,
):
    me = lax.axis_index("kv")
    rows = nb * SB
    depth = tok.shape[1]
    chunks = depth // kc
    spans = rows // CMP
    kvd = G * HD

    def part(i):
        return pl.ds(i * kc, kc)

    def loads(i):
        return [
            pltpu.make_async_copy(tok_hbm.at[:, part(i)], tok.at[:, part(i)], sem_tok.at[i]),
            pltpu.make_async_copy(kw_hbm.at[part(i)], kvw.at[part(i), pl.ds(0, kvd)], sem_kw.at[i]),
            pltpu.make_async_copy(vw_hbm.at[part(i)], kvw.at[part(i), pl.ds(kvd, kvd)], sem_vw.at[i]),
        ]

    def late(i):
        return [
            pltpu.make_async_copy(qw_hbm.at[part(i)], qw.at[part(i)], sem_qw.at[i]),
            pltpu.make_async_copy(gw_hbm.at[part(i)], gw.at[part(i)], sem_gw.at[i]),
        ]

    for i in range(chunks):
        for c in loads(i):
            c.start()
    for i in range(chunks):
        for c in late(i):
            c.start()

    barrier = pltpu.get_barrier_semaphore()
    for i in range(1, n):
        pl.semaphore_signal(
            barrier, inc=1, device_id={"kv": lax.rem(me + i, n)}, device_id_type=MESH
        )
    pl.semaphore_wait(barrier, n - 1)

    def req_copy(i):
        return pltpu.make_async_remote_copy(
            src_ref=req_ref.at[lax.rem(me + n - i, n)], dst_ref=req_in.at[i],
            send_sem=req_s.at[i], recv_sem=req_r.at[i],
            device_id={"kv": lax.rem(me + n - i, n)}, device_id_type=MESH,
        )

    def blk_copy(i):
        return pltpu.make_async_remote_copy(
            src_ref=send.at[i],
            dst_ref=tab_ref.at[pl.ds(G * nb + me * G * 2, G * 2)],
            send_sem=blk_s.at[i], recv_sem=blk_r.at[i],
            device_id={"kv": lax.rem(me + i, n)}, device_id_type=MESH,
        )

    def blk_arrival(i):
        s = lax.rem(me + n - i, n)
        return pltpu.make_async_remote_copy(
            src_ref=send.at[i],
            dst_ref=tab_ref.at[pl.ds(G * nb + s * G * 2, G * 2)],
            send_sem=blk_s.at[i], recv_sem=blk_r.at[i],
            device_id={"kv": lax.rem(me + i, n)}, device_id_type=MESH,
        )

    def sum_copy(i):
        return pltpu.make_async_remote_copy(
            src_ref=sum_send, dst_ref=sum_ref.at[me],
            send_sem=sum_s.at[i], recv_sem=sum_r.at[i],
            device_id={"kv": lax.rem(me + i, n)}, device_id_type=MESH,
        )

    def sum_arrival(i):
        return pltpu.make_async_remote_copy(
            src_ref=sum_send, dst_ref=sum_ref.at[lax.rem(me + n - i, n)],
            send_sem=sum_s.at[i], recv_sem=sum_r.at[i],
            device_id={"kv": lax.rem(me + i, n)}, device_id_type=MESH,
        )

    for i in range(1, n):
        req_copy(i).start()

    acc[:, : 2 * kvd] = jnp.zeros((rows, 2 * kvd), F32)

    def kv_step(i, carry):
        for c in loads(i):
            c.wait()
        acc[:, : 2 * kvd] += jnp.dot(tok[:, part(i)], kvw[part(i), :], preferred_element_type=F32)
        return carry

    lax.fori_loop(0, chunks, kv_step, 0)
    lane = lax.broadcasted_iota(jnp.int32, (SB, LANES), 1)
    lower = lane < HD

    def table_step(b, carry):
        r0 = pl.ds(b * SB, SB)
        for pair in range(G // 2):
            keys = acc[r0, pair * LANES : (pair + 1) * LANES].astype(BF16).astype(F32)
            vals = acc[r0, kvd + pair * LANES : kvd + (pair + 1) * LANES].astype(BF16).astype(F32)
            first = jnp.where(lower, keys, pltpu.roll(vals, HD, 1))
            second = jnp.where(lower, pltpu.roll(keys, HD, 1), vals)
            for g, t in ((2 * pair, first), (2 * pair + 1, second)):
                tf[g, b] = t
                tab_ref[g * nb + b] = t.astype(BF16)
        return carry

    lax.fori_loop(0, nb, table_step, 0)
    for g in range(G):
        t = tf[g].reshape(spans, CMP, LANES)
        w = (t + pos_ref[...][None]) * mix_ref[g][None]
        s = jnp.sum(w, axis=1)
        s = jnp.concatenate([s, jnp.zeros((pad - spans, LANES), F32)], axis=0)
        sum_send[g] = s.astype(BF16)
        sum_ref[me, g] = s.astype(BF16)
    for i in range(1, n):
        sum_copy(i).start()
    for i in range(1, n):
        req_copy(i).wait_recv()

        @pl.when(me + i < n)
        def _():
            wanted = req_in[i]
            for k in range(G * 2):
                g = k // 2
                want = jnp.broadcast_to(wanted[k : k + 1], (SB, LANES))
                block = tf[g, 0]
                for b in range(1, nb):
                    block = jnp.where(want == b, tf[g, b], block)
                send[i, k] = block.astype(BF16)
            blk_copy(i).start()

    acc[...] = jnp.zeros_like(acc)
    gacc[...] = jnp.zeros_like(gacc)

    def q_step(i, carry):
        for c in late(i):
            c.wait()
        acc[...] += jnp.dot(tok[:, part(i)], qw[part(i), :], preferred_element_type=F32)
        gacc[...] += jnp.dot(tok[:, part(i)], gw[part(i), :], preferred_element_type=F32)
        return carry

    lax.fori_loop(0, chunks, q_step, 0)
    gate_ref[...] = jax.nn.sigmoid(gacc[...])

    def query_step(b, carry):
        r0 = pl.ds(b * SB, SB)
        for g in range(G):
            for pair in range(R // 2):
                at = (g * R // 2 + pair) * LANES
                t = acc[r0, at : at + LANES].astype(BF16).astype(F32) * (HD ** -0.5)
                even = jnp.where(lower, t, 0.0)
                odd = jnp.where(lower, pltpu.roll(t, HD, 1), 0.0)
                qp_ref[g, b, 2 * pair * SB : (2 * pair + 1) * SB, :] = even.astype(BF16)
                qp_ref[g, b, (2 * pair + 1) * SB : (2 * pair + 2) * SB, :] = odd.astype(BF16)
        return carry

    lax.fori_loop(0, nb, query_step, 0)
    for i in range(1, n):
        sum_arrival(i).wait_recv()
        sum_copy(i).wait_send()
        req_copy(i).wait_send()

        @pl.when(me + i < n)
        def _():
            blk_copy(i).wait_send()

        @pl.when(me - i >= 0)
        def _():
            blk_arrival(i).wait_recv()


def attend_kernel(
    n, G, R, nb, pad, spans, cw,
    idx_ref, qp_ref, gate_ref, tab_ref, sum_ref, bias_ref, ow_hbm,
    out_ref,
    ow, att, kbuf, mine, dsend, drecv, xsend, xrecv,
    sem_w, d_s, d_r, x_s, x_r,
):
    me = lax.axis_index("kv")
    tp = lax.axis_index("tp")
    core = lax.rem(tp, 2)
    side = tp // 2
    partner = side * 2 + 1 - core
    across = (1 - side) * 2 + core
    rows = nb * SB
    quarter = rows // 4
    half_blocks = nb // 2
    width = out_ref.shape[1]
    chunks = width // cw
    group_rows = R * SB

    load = pltpu.make_async_copy(ow_hbm, ow, sem_w)
    load.start()

    barrier = pltpu.get_barrier_semaphore()
    for peer in (partner, across):
        pl.semaphore_signal(barrier, inc=1, device_id={"tp": peer}, device_id_type=MESH)
    pl.semaphore_wait(barrier, 2)

    row = lax.broadcasted_iota(jnp.int32, (group_rows, LANES), 0) % SB
    lane = lax.broadcasted_iota(jnp.int32, (group_rows, LANES), 1)
    tri = jnp.where((lane < SB) & (lane > row), LOW, 0.0)
    span_lane = lax.broadcasted_iota(jnp.int32, (group_rows, n * pad), 1)
    span_in = span_lane % pad
    span_end = ((span_lane // pad) * spans + span_in) * CMP + (CMP - 1)
    span_row = lax.broadcasted_iota(jnp.int32, (group_rows, n * pad), 0) % SB
    low64 = lax.broadcasted_iota(jnp.int32, (SB, LANES), 1) < HD
    gate_lane = lax.broadcasted_iota(jnp.int32, (SB, gate_ref.shape[1]), 1)
    nt = (((1,), (1,)), ((), ()))

    def attend(b, carry):
        gates = gate_ref[pl.ds(b * SB, SB), :]
        seen = (span_in < spans) & (span_end - span_row <= me * rows + b * SB)
        for g in range(G):
            base = (b * G + g) * N_SEL
            for j in range(N_SEL):
                kbuf[g, j * SB : (j + 1) * SB, :] = tab_ref[idx_ref[base + j]]
            kb = kbuf[g]
            q = qp_ref[g, b]
            s = lax.dot_general(q, kb, nt, preferred_element_type=F32)
            s = s + bias_ref[b * G + g]
            s = jnp.concatenate([s[:, :LANES] + tri, s[:, LANES:]], axis=1)
            m = jnp.max(s, axis=-1, keepdims=True)
            p = jnp.exp(s - m)
            l = jnp.sum(p, axis=-1, keepdims=True)
            oc = jnp.dot(p.astype(BF16), kb, preferred_element_type=F32)
            sm = sum_ref[:, g].reshape(n * pad, LANES)
            s2 = lax.dot_general(q, sm, nt, preferred_element_type=F32)
            s2 = jnp.where(seen, s2, LOW)
            m2 = jnp.max(s2, axis=-1, keepdims=True)
            p2 = jnp.where(seen, jnp.exp(s2 - m2), 0.0)
            l2 = jnp.sum(p2, axis=-1, keepdims=True)
            os = jnp.dot(p2.astype(BF16), sm, preferred_element_type=F32)
            ic = 1.0 / l
            i2 = jnp.where(l2 > 0.0, 1.0 / jnp.where(l2 > 0.0, l2, 1.0), 0.0)
            parts = []
            for r in range(R):
                at = (tp * G * R + g * R + r) * 2
                g0 = jnp.sum(jnp.where(gate_lane == at, gates, 0.0), axis=-1, keepdims=True)
                g1 = jnp.sum(jnp.where(gate_lane == at + 1, gates, 0.0), axis=-1, keepdims=True)
                k = slice(r * SB, (r + 1) * SB)
                parts.append(os[k] * (g0 * i2[k]) + oc[k] * (g1 * ic[k]))
            for pair in range(R // 2):
                t = jnp.where(low64, pltpu.roll(parts[2 * pair], HD, 1), parts[2 * pair + 1])
                at = (g * R // 2 + pair) * LANES
                att[pl.ds(b * SB, SB), at : at + LANES] = t.astype(BF16)
        return carry

    def d_copy(h, j):
        return pltpu.make_async_remote_copy(
            src_ref=dsend.at[h, j], dst_ref=drecv.at[h, j],
            send_sem=d_s.at[h, j], recv_sem=d_r.at[h, j],
            device_id={"tp": partner}, device_id_type=MESH,
        )

    def x_copy(j):
        return pltpu.make_async_remote_copy(
            src_ref=xsend.at[j], dst_ref=xrecv.at[j],
            send_sem=x_s.at[j], recv_sem=x_r.at[j],
            device_id={"tp": across}, device_id_type=MESH,
        )

    def product(h, first_row, j):
        cols = pl.ds(pl.multiple_of(j * cw, cw), cw)
        w = ow[:, cols]
        theirs = att[pl.ds(first_row + (1 - core) * quarter, quarter), :]
        dsend[h, j] = jnp.dot(theirs, w, preferred_element_type=F32).astype(BF16)
        d_copy(h, j).start()
        ours = att[pl.ds(first_row + core * quarter, quarter), :]
        mine[h, j] = jnp.dot(ours, w, preferred_element_type=F32).astype(BF16)

    def forward(j):
        d_copy(0, j).wait_recv()
        xsend[j] = (mine[0, j].astype(F32) + drecv[0, j].astype(F32)).astype(BF16)
        x_copy(j).start()

    other_first = (1 - side) * half_blocks
    lax.fori_loop(other_first, other_first + half_blocks, attend, 0)
    load.wait()
    product(0, other_first * SB, 0)

    def first_step(j, carry):
        product(0, other_first * SB, j)
        forward(j - 1)
        return carry

    lax.fori_loop(1, chunks, first_step, 0)
    forward(chunks - 1)

    own_first = side * half_blocks
    lax.fori_loop(own_first, own_first + half_blocks, attend, 0)

    def second_step(j, carry):
        product(1, own_first * SB, j)
        return carry

    lax.fori_loop(0, chunks, second_step, 0)

    def last_step(j, carry):
        cols = pl.ds(pl.multiple_of(j * cw, cw), cw)
        d_copy(1, j).wait_recv()
        x_copy(j).wait_recv()
        total = mine[1, j].astype(F32) + drecv[1, j].astype(F32) + xrecv[j].astype(F32)
        out_ref[:, cols] = total.astype(BF16)
        d_copy(0, j).wait_send()
        d_copy(1, j).wait_send()
        x_copy(j).wait_send()
        return carry

    lax.fori_loop(0, chunks, last_step, 0)


def local(
    n,
    tokens, query_weight, key_weight, value_weight, gate_weight,
    summary_pos, key_mixing, value_mixing, out_weight, chosen,
):
    rows, depth = tokens.shape
    me = lax.axis_index("kv")
    tp = lax.axis_index("tp")
    heads = query_weight.shape[1] // HD
    G = key_weight.shape[1] // HD
    R = heads // G
    nb = rows // SB
    spans = rows // CMP
    pad = -(-spans // 16) * 16
    kc = min(1024, depth)
    chunks = depth // kc
    width = out_weight.shape[1]
    cw = 512
    oc = width // cw
    gates_all = gate_weight.shape[1]

    source = chosen // nb
    inside = chosen - source * nb
    hit = source[None] == jnp.arange(n, dtype=jnp.int32)[:, None, None, None]
    lo = jnp.min(jnp.where(hit, inside[None], nb), axis=(1, 3))
    hi = jnp.max(jnp.where(hit, inside[None], -1), axis=(1, 3))
    lo = jnp.where(lo == nb, 0, lo)
    hi = jnp.where(hi < 0, 0, hi)
    req = jnp.stack([lo, hi], axis=-1).reshape(n, G * 2)
    req = jnp.pad(req, ((0, 0), (0, 8 - G * 2)))
    req = jnp.broadcast_to(req[:, :, None], (n, 8, LANES))
    low_of = jnp.sum(jnp.where(hit, lo[:, None, :, None], 0), axis=0)
    head = jnp.arange(G, dtype=jnp.int32)[None, :, None]
    away = G * nb + (source * G + head) * 2 + (inside != low_of).astype(jnp.int32)
    index = jnp.where(source == me, head * nb + inside, away).reshape(-1)
    bias = jnp.where(first_named(chosen), 0.0, LOW)
    bias = jnp.broadcast_to(bias[..., None], (nb, G, N_SEL, SB)).reshape(nb * G, 1, N_SEL * SB)

    km = lax.dynamic_slice_in_dim(key_mixing, tp * G, G, 1).astype(F32).T
    vm = lax.dynamic_slice_in_dim(value_mixing, tp * G, G, 1).astype(F32).T
    mix = jnp.concatenate(
        [
            jnp.broadcast_to(km[:, :, None], (G, CMP, HD)),
            jnp.broadcast_to(vm[:, :, None], (G, CMP, HD)),
        ],
        axis=-1,
    )
    pos = jnp.concatenate([summary_pos, summary_pos], axis=-1).astype(F32)

    vmem = pl.BlockSpec(memory_space=pltpu.VMEM)
    hbm = pl.BlockSpec(memory_space=pl.ANY)
    smem = pl.BlockSpec(memory_space=pltpu.SMEM)
    dma = pltpu.SemaphoreType.DMA
    table = G * nb + n * G * 2
    queries, gates, tab, summary = pl.pallas_call(
        functools.partial(project_kernel, n, G, R, nb, kc, pad),
        name="project",
        out_shape=[
            jax.ShapeDtypeStruct((G, nb, R * SB, LANES), BF16),
            jax.ShapeDtypeStruct((rows, gates_all), F32),
            jax.ShapeDtypeStruct((table, SB, LANES), BF16),
            jax.ShapeDtypeStruct((n, G, pad, LANES), BF16),
        ],
        in_specs=[hbm] * 5 + [vmem] * 3,
        out_specs=[vmem] * 4,
        scratch_shapes=[
            pltpu.VMEM((rows, depth), BF16),
            pltpu.VMEM((depth, heads * HD), BF16),
            pltpu.VMEM((depth, 2 * G * HD), BF16),
            pltpu.VMEM((depth, gates_all), BF16),
            pltpu.VMEM((rows, heads * HD), F32),
            pltpu.VMEM((rows, gates_all), F32),
            pltpu.VMEM((G, nb, SB, LANES), F32),
            pltpu.VMEM((n, 8, LANES), jnp.int32),
            pltpu.VMEM((n, G * 2, SB, LANES), BF16),
            pltpu.VMEM((G, pad, LANES), BF16),
            dma((chunks,)), dma((chunks,)), dma((chunks,)), dma((chunks,)), dma((chunks,)),
            dma((n,)), dma((n,)), dma((n,)), dma((n,)), dma((n,)), dma((n,)),
        ],
        compiler_params=pltpu.CompilerParams(
            collective_id=1, has_side_effects=True, vmem_limit_bytes=VMEM_LIMIT
        ),
    )(tokens, query_weight, key_weight, value_weight, gate_weight, req, mix, pos)

    quarter = rows // 4
    return pl.pallas_call(
        functools.partial(attend_kernel, n, G, R, nb, pad, spans, cw),
        name="attend",
        out_shape=jax.ShapeDtypeStruct((quarter, width), BF16),
        in_specs=[smem] + [vmem] * 5 + [hbm],
        out_specs=vmem,
        scratch_shapes=[
            pltpu.VMEM(out_weight.shape, BF16),
            pltpu.VMEM((rows, heads * HD), BF16),
            pltpu.VMEM((G, N_SEL * SB, LANES), BF16),
            pltpu.VMEM((2, oc, quarter, cw), BF16),
            pltpu.VMEM((2, oc, quarter, cw), BF16),
            pltpu.VMEM((2, oc, quarter, cw), BF16),
            pltpu.VMEM((oc, quarter, cw), BF16),
            pltpu.VMEM((oc, quarter, cw), BF16),
            dma, dma((2, oc)), dma((2, oc)), dma((oc,)), dma((oc,)),
        ],
        compiler_params=pltpu.CompilerParams(
            collective_id=2, has_side_effects=True, vmem_limit_bytes=VMEM_LIMIT
        ),
    )(index, queries, gates, tab, summary, bias, out_weight)


def solution(mesh):
    placed = (
        P("kv", None),
        P(None, "tp"),
        P(None, "tp"),
        P(None, "tp"),
        P(),
        P(),
        P(),
        P(),
        P("tp", None),
        P("kv", "tp", None),
    )
    return jax.shard_map(
        functools.partial(local, mesh.shape["kv"]),
        mesh=mesh, in_specs=placed, out_specs=P(("kv", "tp"), None), check_vma=False,
    )
```

```python
import functools

import jax
import jax.numpy as jnp
from jax import lax
from jax.experimental import pallas as pl
from jax.experimental.pallas import tpu as pltpu
from jax.sharding import PartitionSpec as P

HD = 64
CMP = 32
SB = 64
N_SEL = 16
LANES = 128
LOW = -1e30
F32 = jnp.float32
BF16 = jnp.bfloat16
MESH = pl.DeviceIdType.MESH
VMEM_LIMIT = 64_000_000


def project_kernel(
    n, G, R, nb, kc, pad,
    tok_hbm, qw_hbm, kw_hbm, vw_hbm, gw_hbm, ch_ref, km_ref, vm_ref, pos_in,
    qp_ref, gate_ref, tab_ref, sum_ref, idx_ref, bias_ref,
    tok, qw, kvw, gw, acc, gacc, tf, named, pos_ref, req_ref, req_in, send, sum_send,
    sem_tok, sem_kw, sem_vw, sem_qw, sem_gw,
    req_s, req_r, blk_s, blk_r, sum_s, sum_r,
):
    me = lax.axis_index("kv")
    rows = nb * SB
    depth = tok.shape[1]
    chunks = depth // kc
    spans = rows // CMP
    kvd = G * HD

    def part(i):
        return pl.ds(i * kc, kc)

    def loads(i):
        return [
            pltpu.make_async_copy(tok_hbm.at[:, part(i)], tok.at[:, part(i)], sem_tok.at[i]),
            pltpu.make_async_copy(kw_hbm.at[part(i)], kvw.at[part(i), pl.ds(0, kvd)], sem_kw.at[i]),
            pltpu.make_async_copy(vw_hbm.at[part(i)], kvw.at[part(i), pl.ds(kvd, kvd)], sem_vw.at[i]),
        ]

    def late(i):
        return [
            pltpu.make_async_copy(qw_hbm.at[part(i)], qw.at[part(i)], sem_qw.at[i]),
            pltpu.make_async_copy(gw_hbm.at[:, part(i)], gw.at[:, part(i)], sem_gw.at[i]),
        ]

    for i in range(chunks):
        for c in loads(i):
            c.start()
    for i in range(chunks):
        for c in late(i):
            c.start()

    barrier = pltpu.get_barrier_semaphore()
    for i in range(1, n):
        pl.semaphore_signal(
            barrier, inc=1, device_id={"kv": lax.rem(me + i, n)}, device_id_type=MESH
        )

    place = lax.broadcasted_iota(jnp.int32, named.shape, 1)
    slot_row = lax.broadcasted_iota(jnp.int32, (LANES, N_SEL * SB), 0)
    slot_col = lax.broadcasted_iota(jnp.int32, (LANES, N_SEL * SB), 1) // SB
    spread = jnp.where(slot_row == slot_col, 1.0, 0.0).astype(BF16)
    for g in range(G):
        named[...] = jnp.full(named.shape, -1.0, F32)
        named[:nb, :N_SEL] = ch_ref[:, g, :].astype(F32)
        c = named[...]
        source = jnp.zeros_like(c)
        for s in range(1, n):
            source = source + jnp.where(c >= s * nb, 1.0, 0.0)
        inside = c - source * nb
        low_of = jnp.zeros_like(c)
        for s in range(n):
            hit = (c >= 0.0) & (source == s)
            lo = jnp.where(hit, inside, float(nb))
            lo = jnp.min(jnp.min(lo, axis=0, keepdims=True), axis=1, keepdims=True)
            lo = jnp.where(lo == nb, 0.0, lo)
            hi = jnp.where(hit, inside, 0.0)
            hi = jnp.max(jnp.max(hi, axis=0, keepdims=True), axis=1, keepdims=True)
            low_of = jnp.where(hit, lo, low_of)
            req_ref[s, 2 * g : 2 * g + 1] = jnp.broadcast_to(lo, (1, LANES))
            req_ref[s, 2 * g + 1 : 2 * g + 2] = jnp.broadcast_to(hi, (1, LANES))
        away = G * nb + (source * G + g) * 2 + jnp.where(inside != low_of, 1.0, 0.0)
        at = jnp.where(source == me.astype(F32), g * nb + inside, away)
        idx_ref[g] = at[:nb, :N_SEL].astype(jnp.int32)
        again = jnp.zeros_like(c)
        for d in range(1, N_SEL):
            again = jnp.where((place >= d) & (pltpu.roll(c, d, 1) == c), 1.0, again)
        bias_ref[g] = jnp.dot(again.astype(BF16), spread, preferred_element_type=F32) * LOW

    pl.semaphore_wait(barrier, n - 1)

    def req_copy(i):
        return pltpu.make_async_remote_copy(
            src_ref=req_ref.at[lax.rem(me + n - i, n)], dst_ref=req_in.at[i],
            send_sem=req_s.at[i], recv_sem=req_r.at[i],
            device_id={"kv": lax.rem(me + n - i, n)}, device_id_type=MESH,
        )

    def blk_copy(i):
        return pltpu.make_async_remote_copy(
            src_ref=send.at[i],
            dst_ref=tab_ref.at[pl.ds(G * nb + me * G * 2, G * 2)],
            send_sem=blk_s.at[i], recv_sem=blk_r.at[i],
            device_id={"kv": lax.rem(me + i, n)}, device_id_type=MESH,
        )

    def blk_arrival(i):
        s = lax.rem(me + n - i, n)
        return pltpu.make_async_remote_copy(
            src_ref=send.at[i],
            dst_ref=tab_ref.at[pl.ds(G * nb + s * G * 2, G * 2)],
            send_sem=blk_s.at[i], recv_sem=blk_r.at[i],
            device_id={"kv": lax.rem(me + i, n)}, device_id_type=MESH,
        )

    def sum_copy(i):
        return pltpu.make_async_remote_copy(
            src_ref=sum_send, dst_ref=sum_ref.at[me],
            send_sem=sum_s.at[i], recv_sem=sum_r.at[i],
            device_id={"kv": lax.rem(me + i, n)}, device_id_type=MESH,
        )

    def sum_arrival(i):
        return pltpu.make_async_remote_copy(
            src_ref=sum_send, dst_ref=sum_ref.at[lax.rem(me + n - i, n)],
            send_sem=sum_s.at[i], recv_sem=sum_r.at[i],
            device_id={"kv": lax.rem(me + i, n)}, device_id_type=MESH,
        )

    for i in range(1, n):
        req_copy(i).start()

    acc[:, : 2 * kvd] = jnp.zeros((rows, 2 * kvd), F32)

    def kv_step(i, carry):
        for c in loads(i):
            c.wait()
        acc[:, : 2 * kvd] += jnp.dot(tok[:, part(i)], kvw[part(i), :], preferred_element_type=F32)
        return carry

    lax.fori_loop(0, chunks, kv_step, 0)
    lane = lax.broadcasted_iota(jnp.int32, (SB, LANES), 1)
    lower = lane < HD

    def table_step(b, carry):
        r0 = pl.ds(b * SB, SB)
        for pair in range(G // 2):
            keys = acc[r0, pair * LANES : (pair + 1) * LANES].astype(BF16).astype(F32)
            vals = acc[r0, kvd + pair * LANES : kvd + (pair + 1) * LANES].astype(BF16).astype(F32)
            first = jnp.where(lower, keys, pltpu.roll(vals, HD, 1))
            second = jnp.where(lower, pltpu.roll(keys, HD, 1), vals)
            for g, t in ((2 * pair, first), (2 * pair + 1, second)):
                tf[g, b] = t
                tab_ref[g * nb + b] = t.astype(BF16)
        return carry

    lax.fori_loop(0, nb, table_step, 0)
    pos_ref[:, :HD] = pos_in[...].astype(F32)
    pos_ref[:, HD:] = pos_in[...].astype(F32)
    mix_row = lax.broadcasted_iota(jnp.int32, km_ref.shape, 0)
    mix_low = lax.broadcasted_iota(jnp.int32, (CMP, LANES), 1) < HD
    diagonal = lax.broadcasted_iota(jnp.int32, (CMP, CMP), 0) == lax.broadcasted_iota(
        jnp.int32, (CMP, CMP), 1
    )

    def mix_column(ref, head):
        line = jnp.where(mix_row == head, ref[...].astype(F32), 0.0)
        line = jnp.sum(line, axis=0, keepdims=True)
        return jnp.sum(jnp.where(diagonal, line, 0.0), axis=1, keepdims=True)

    for g in range(G):
        head = lax.axis_index("tp") * G + g
        km = mix_column(km_ref, head)
        vm = mix_column(vm_ref, head)
        mix = jnp.where(mix_low, km, vm)
        t = tf[g].reshape(spans, CMP, LANES)
        w = (t + pos_ref[...][None]) * mix[None]
        s = jnp.sum(w, axis=1)
        s = jnp.concatenate([s, jnp.zeros((pad - spans, LANES), F32)], axis=0)
        sum_send[g] = s.astype(BF16)
        sum_ref[me, g] = s.astype(BF16)
    for i in range(1, n):
        sum_copy(i).start()
    for i in range(1, n):
        req_copy(i).wait_recv()

        @pl.when(me + i < n)
        def _():
            wanted = req_in[i]
            for k in range(G * 2):
                g = k // 2
                want = jnp.broadcast_to(wanted[k : k + 1], (SB, LANES))
                block = tf[g, 0]
                for b in range(1, nb):
                    block = jnp.where(want == float(b), tf[g, b], block)
                send[i, k] = block.astype(BF16)
            blk_copy(i).start()

    acc[...] = jnp.zeros_like(acc)
    gacc[...] = jnp.zeros_like(gacc)

    def q_step(i, carry):
        for c in late(i):
            c.wait()
        acc[...] += jnp.dot(tok[:, part(i)], qw[part(i), :], preferred_element_type=F32)
        gacc[...] += lax.dot_general(
            tok[:, part(i)], gw[:, part(i)], (((1,), (1,)), ((), ())), preferred_element_type=F32
        )
        return carry

    lax.fori_loop(0, chunks, q_step, 0)
    gate_ref[...] = jax.nn.sigmoid(gacc[...])

    def query_step(b, carry):
        r0 = pl.ds(b * SB, SB)
        for g in range(G):
            for pair in range(R // 2):
                at = (g * R // 2 + pair) * LANES
                t = acc[r0, at : at + LANES].astype(BF16).astype(F32) * (HD ** -0.5)
                even = jnp.where(lower, t, 0.0)
                odd = jnp.where(lower, pltpu.roll(t, HD, 1), 0.0)
                qp_ref[g, b, 2 * pair * SB : (2 * pair + 1) * SB, :] = even.astype(BF16)
                qp_ref[g, b, (2 * pair + 1) * SB : (2 * pair + 2) * SB, :] = odd.astype(BF16)
        return carry

    lax.fori_loop(0, nb, query_step, 0)
    for i in range(1, n):
        sum_arrival(i).wait_recv()
        sum_copy(i).wait_send()
        req_copy(i).wait_send()

        @pl.when(me + i < n)
        def _():
            blk_copy(i).wait_send()

        @pl.when(me - i >= 0)
        def _():
            blk_arrival(i).wait_recv()


def attend_kernel(
    n, G, R, nb, pad, spans, cw,
    idx_ref, qp_ref, gate_ref, tab_ref, sum_ref, bias_ref, ow_hbm,
    out_ref,
    ow, att, kbuf, mine, dsend, drecv, early, esend, erecv, xsend, xrecv, base,
    sem_w, d_s, d_r, e_s, e_r, x_s, x_r,
):
    me = lax.axis_index("kv")
    tp = lax.axis_index("tp")
    core = lax.rem(tp, 2)
    side = tp // 2
    partner = side * 2 + 1 - core
    rows = nb * SB
    quarter = rows // 4
    half_blocks = nb // 2
    width = out_ref.shape[1]
    chunks = width // cw
    group_rows = R * SB
    side_cols = width // 2
    step_rows = SB // 2

    load = pltpu.make_async_copy(ow_hbm, ow, sem_w)
    load.start()

    barrier = pltpu.get_barrier_semaphore()
    for i in range(1, 4):
        pl.semaphore_signal(barrier, inc=1, device_id={"tp": lax.rem(tp + i, 4)}, device_id_type=MESH)
    pl.semaphore_wait(barrier, 3)

    row = lax.broadcasted_iota(jnp.int32, (group_rows, LANES), 0) % SB
    lane = lax.broadcasted_iota(jnp.int32, (group_rows, LANES), 1)
    tri = jnp.where((lane < SB) & (lane > row), LOW, 0.0)
    span_lane = lax.broadcasted_iota(jnp.int32, (group_rows, n * pad), 1)
    span_in = span_lane % pad
    span_end = ((span_lane // pad) * spans + span_in) * CMP + (CMP - 1)
    span_row = lax.broadcasted_iota(jnp.int32, (group_rows, n * pad), 0) % SB
    low64 = lax.broadcasted_iota(jnp.int32, (SB, LANES), 1) < HD
    gate_lane = lax.broadcasted_iota(jnp.int32, (SB, gate_ref.shape[1]), 1)
    nt = (((1,), (1,)), ((), ()))

    def attend(b, carry):
        gates = gate_ref[pl.ds(b * SB, SB), :]
        seen = (span_in < spans) & (span_end - span_row <= me * rows + b * SB)
        for g in range(G):
            for j in range(N_SEL):
                kbuf[g, j * SB : (j + 1) * SB, :] = tab_ref[idx_ref[g, b, j]]
            kb = kbuf[g]
            q = qp_ref[g, b]
            s = lax.dot_general(q, kb, nt, preferred_element_type=F32)
            s = s + bias_ref[g, pl.ds(b, 1), :]
            s = jnp.concatenate([s[:, :LANES] + tri, s[:, LANES:]], axis=1)
            m = jnp.max(s, axis=-1, keepdims=True)
            p = jnp.exp(s - m)
            l = jnp.sum(p, axis=-1, keepdims=True)
            oc = jnp.dot(p.astype(BF16), kb, preferred_element_type=F32)
            sm = sum_ref[:, g].reshape(n * pad, LANES)
            s2 = lax.dot_general(q, sm, nt, preferred_element_type=F32)
            s2 = jnp.where(seen, s2, LOW)
            m2 = jnp.max(s2, axis=-1, keepdims=True)
            p2 = jnp.where(seen, jnp.exp(s2 - m2), 0.0)
            l2 = jnp.sum(p2, axis=-1, keepdims=True)
            os = jnp.dot(p2.astype(BF16), sm, preferred_element_type=F32)
            ic = 1.0 / l
            i2 = jnp.where(l2 > 0.0, 1.0 / jnp.where(l2 > 0.0, l2, 1.0), 0.0)
            parts = []
            for r in range(R):
                at = (tp * G * R + g * R + r) * 2
                g0 = jnp.sum(jnp.where(gate_lane == at, gates, 0.0), axis=-1, keepdims=True)
                g1 = jnp.sum(jnp.where(gate_lane == at + 1, gates, 0.0), axis=-1, keepdims=True)
                k = slice(r * SB, (r + 1) * SB)
                parts.append(os[k] * (g0 * i2[k]) + oc[k] * (g1 * ic[k]))
            for pair in range(R // 2):
                t = jnp.where(low64, pltpu.roll(parts[2 * pair], HD, 1), parts[2 * pair + 1])
                at = (g * R // 2 + pair) * LANES
                att[pl.ds(b * SB, SB), at : at + LANES] = t.astype(BF16)
        return carry

    def d_copy(j):
        return pltpu.make_async_remote_copy(
            src_ref=dsend.at[j], dst_ref=drecv.at[j],
            send_sem=d_s.at[j], recv_sem=d_r.at[j],
            device_id={"tp": partner}, device_id_type=MESH,
        )

    def e_copy(i):
        return pltpu.make_async_remote_copy(
            src_ref=esend.at[i], dst_ref=erecv.at[i],
            send_sem=e_s.at[i], recv_sem=e_r.at[i],
            device_id={"tp": partner}, device_id_type=MESH,
        )

    def x_copy(k):
        step = lax.rem(k, half_blocks)
        return pltpu.make_async_remote_copy(
            src_ref=xsend.at[k], dst_ref=xrecv.at[core, step],
            send_sem=x_s.at[k], recv_sem=x_r.at[core, step],
            device_id={"tp": (1 - side) * 2 + k // half_blocks}, device_id_type=MESH,
        )

    def x_arrival(c, step):
        return pltpu.make_async_remote_copy(
            src_ref=xsend.at[step], dst_ref=xrecv.at[c, step],
            send_sem=x_s.at[step], recv_sem=x_r.at[c, step],
            device_id={"tp": (1 - side) * 2 + core}, device_id_type=MESH,
        )

    other_first = (1 - side) * half_blocks

    def early_block(i):
        attend(other_first + i, 0)
        a = att[pl.ds((other_first + i) * SB, SB), :]
        for j in range(side_cols // cw):
            cols = pl.ds(pl.multiple_of((1 - core) * side_cols + j * cw, cw), cw)
            esend[i, :, j * cw : (j + 1) * cw] = jnp.dot(
                a, ow[:, cols], preferred_element_type=F32
            ).astype(BF16)
        e_copy(i).start()
        for j in range(side_cols // cw):
            cols = pl.ds(pl.multiple_of(core * side_cols + j * cw, cw), cw)
            early[i, :, j * cw : (j + 1) * cw] = jnp.dot(
                a, ow[:, cols], preferred_element_type=F32
            ).astype(BF16)

    def forward(i):
        e_copy(i).wait_recv()
        for k in range(2):
            r = slice(k * step_rows, (k + 1) * step_rows)
            xsend[2 * i + k] = (early[i, r].astype(F32) + erecv[i, r].astype(F32)).astype(BF16)
            x_copy(2 * i + k).start()

    load.wait()

    def early_step(i, carry):
        early_block(i)
        forward(i)
        return carry

    lax.fori_loop(0, half_blocks, early_step, 0)

    own_first = side * half_blocks
    lax.fori_loop(own_first, own_first + half_blocks, attend, 0)

    def own_step(j, carry):
        w = ow[:, pl.ds(pl.multiple_of(j * cw, cw), cw)]
        theirs = att[pl.ds(own_first * SB + (1 - core) * quarter, quarter), :]
        dsend[j] = jnp.dot(theirs, w, preferred_element_type=F32).astype(BF16)
        d_copy(j).start()
        ours = att[pl.ds(own_first * SB + core * quarter, quarter), :]
        mine[j] = jnp.dot(ours, w, preferred_element_type=F32).astype(BF16)
        return carry

    lax.fori_loop(0, chunks, own_step, 0)

    def base_step(j, carry):
        d_copy(j).wait_recv()
        cols = pl.ds(pl.multiple_of(j * cw, cw), cw)
        base[:, cols] = mine[j].astype(F32) + drecv[j].astype(F32)
        d_copy(j).wait_send()
        return carry

    lax.fori_loop(0, chunks, base_step, 0)

    def last_step(k, carry):
        r = pl.ds(pl.multiple_of(k * step_rows, step_rows), step_rows)
        for c in range(2):
            x_arrival(c, k).wait_recv()
            cols = slice(c * side_cols, (c + 1) * side_cols)
            out_ref[r, cols] = (base[r, cols] + xrecv[c, k].astype(F32)).astype(BF16)
        e_copy(k).wait_send()
        x_copy(k).wait_send()
        x_copy(half_blocks + k).wait_send()
        return carry

    lax.fori_loop(0, half_blocks, last_step, 0)


def local(
    n,
    tokens, query_weight, key_weight, value_weight, gate_weight,
    summary_pos, key_mixing, value_mixing, out_weight, chosen,
):
    rows, depth = tokens.shape
    heads = query_weight.shape[1] // HD
    G = key_weight.shape[1] // HD
    R = heads // G
    nb = rows // SB
    spans = rows // CMP
    pad = -(-spans // 16) * 16
    kc = min(1024, depth)
    chunks = depth // kc
    width = out_weight.shape[1]
    cw = 512
    oc = width // cw
    gates_all = gate_weight.shape[1]

    vmem = pl.BlockSpec(memory_space=pltpu.VMEM)
    hbm = pl.BlockSpec(memory_space=pl.ANY)
    smem = pl.BlockSpec(memory_space=pltpu.SMEM)
    dma = pltpu.SemaphoreType.DMA
    table = G * nb + n * G * 2
    nbp = -(-nb // 8) * 8
    queries, gates, tab, summary, index, bias = pl.pallas_call(
        functools.partial(project_kernel, n, G, R, nb, kc, pad),
        name="project",
        out_shape=[
            jax.ShapeDtypeStruct((G, nb, R * SB, LANES), BF16),
            jax.ShapeDtypeStruct((rows, gates_all), F32),
            jax.ShapeDtypeStruct((table, SB, LANES), BF16),
            jax.ShapeDtypeStruct((n, G, pad, LANES), BF16),
            jax.ShapeDtypeStruct((G, nb, N_SEL), jnp.int32),
            jax.ShapeDtypeStruct((G, nbp, N_SEL * SB), F32),
        ],
        in_specs=[hbm] * 5 + [vmem] * 4,
        out_specs=[vmem] * 6,
        scratch_shapes=[
            pltpu.VMEM((rows, depth), BF16),
            pltpu.VMEM((depth, heads * HD), BF16),
            pltpu.VMEM((depth, 2 * G * HD), BF16),
            pltpu.VMEM((gates_all, depth), BF16),
            pltpu.VMEM((rows, heads * HD), F32),
            pltpu.VMEM((rows, gates_all), F32),
            pltpu.VMEM((G, nb, SB, LANES), F32),
            pltpu.VMEM((nbp, LANES), F32),
            pltpu.VMEM((CMP, LANES), F32),
            pltpu.VMEM((n, 8, LANES), F32),
            pltpu.VMEM((n, 8, LANES), F32),
            pltpu.VMEM((n, G * 2, SB, LANES), BF16),
            pltpu.VMEM((G, pad, LANES), BF16),
            dma((chunks,)), dma((chunks,)), dma((chunks,)), dma((chunks,)), dma((chunks,)),
            dma((n,)), dma((n,)), dma((n,)), dma((n,)), dma((n,)), dma((n,)),
        ],
        compiler_params=pltpu.CompilerParams(
            collective_id=1, has_side_effects=True, vmem_limit_bytes=VMEM_LIMIT
        ),
    )(
        tokens, query_weight, key_weight, value_weight, gate_weight.T,
        chosen, key_mixing.T, value_mixing.T, summary_pos,
    )

    quarter = rows // 4
    half = nb // 2
    return pl.pallas_call(
        functools.partial(attend_kernel, n, G, R, nb, pad, spans, cw),
        name="attend",
        out_shape=jax.ShapeDtypeStruct((quarter, width), BF16),
        in_specs=[smem] + [vmem] * 5 + [hbm],
        out_specs=vmem,
        scratch_shapes=[
            pltpu.VMEM(out_weight.shape, BF16),
            pltpu.VMEM((rows, heads * HD), BF16),
            pltpu.VMEM((G, N_SEL * SB, LANES), BF16),
            pltpu.VMEM((oc, quarter, cw), BF16),
            pltpu.VMEM((oc, quarter, cw), BF16),
            pltpu.VMEM((oc, quarter, cw), BF16),
            pltpu.VMEM((half, SB, width // 2), BF16),
            pltpu.VMEM((half, SB, width // 2), BF16),
            pltpu.VMEM((half, SB, width // 2), BF16),
            pltpu.VMEM((2 * half, SB // 2, width // 2), BF16),
            pltpu.VMEM((2, half, SB // 2, width // 2), BF16),
            pltpu.VMEM((quarter, width), F32),
            dma, dma((oc,)), dma((oc,)), dma((half,)), dma((half,)), dma((2 * half,)), dma((2, half)),
        ],
        compiler_params=pltpu.CompilerParams(
            collective_id=2, has_side_effects=True, vmem_limit_bytes=VMEM_LIMIT
        ),
    )(index, queries, gates, tab, summary, bias, out_weight)


def solution(mesh):
    placed = (
        P("kv", None),
        P(None, "tp"),
        P(None, "tp"),
        P(None, "tp"),
        P(),
        P(),
        P(),
        P(),
        P("tp", None),
        P("kv", "tp", None),
    )
    return jax.shard_map(
        functools.partial(local, mesh.shape["kv"]),
        mesh=mesh, in_specs=placed, out_specs=P(("kv", "tp"), None), check_vma=False,
    )
```

```python
import functools

import jax
import jax.numpy as jnp
from jax import lax
from jax.experimental import pallas as pl
from jax.experimental.pallas import tpu as pltpu
from jax.sharding import PartitionSpec as P

HD = 64
CMP = 32
SB = 64
N_SEL = 16
LANES = 128
LOW = -1e30
F32 = jnp.float32
BF16 = jnp.bfloat16
MESH = pl.DeviceIdType.MESH
VMEM_LIMIT = 64_000_000


def project(
    n, G, R, nb, kc, pad, ow_load, idx_smem, sem_idx,
    tok_hbm, qw_hbm, kw_hbm, vw_hbm, gw_hbm, ch_ref, km_ref, vm_ref, pos_in,
    qp_ref, gate_ref, tab_ref, sum_ref, idx_ref, bias_ref,
    tok, qw, kvw, gw, acc, gacc, tf, named, pos_ref, req_ref, req_in, req_smem, sem_req, send, sum_send,
    sem_tok, sem_kw, sem_vw, sem_qw, sem_gw,
    req_s, req_r, blk_s, blk_r, sum_s, sum_r,
):
    tp = lax.axis_index("tp")
    me = lax.axis_index("kv")
    rows = nb * SB
    depth = tok.shape[1]
    chunks = depth // kc
    spans = rows // CMP
    kvd = G * HD

    def part(i):
        return pl.ds(i * kc, kc)

    def loads(i):
        return [
            pltpu.make_async_copy(tok_hbm.at[:, part(i)], tok.at[:, part(i)], sem_tok.at[i]),
            pltpu.make_async_copy(kw_hbm.at[part(i)], kvw.at[part(i), pl.ds(0, kvd)], sem_kw.at[i]),
            pltpu.make_async_copy(vw_hbm.at[part(i)], kvw.at[part(i), pl.ds(kvd, kvd)], sem_vw.at[i]),
        ]

    def late(i):
        return [
            pltpu.make_async_copy(qw_hbm.at[part(i)], qw.at[part(i)], sem_qw.at[i]),
            pltpu.make_async_copy(gw_hbm.at[:, part(i)], gw.at[:, part(i)], sem_gw.at[i]),
        ]

    for i in range(chunks):
        for c in loads(i):
            c.start()
    for i in range(chunks):
        for c in late(i):
            c.start()
    ow_load.start()

    barrier = pltpu.get_barrier_semaphore()
    for i in range(1, n):
        pl.semaphore_signal(
            barrier, inc=1, device_id={"kv": lax.rem(me + i, n)}, device_id_type=MESH
        )
    for i in range(1, 4):
        pl.semaphore_signal(barrier, inc=1, device_id={"tp": lax.rem(tp + i, 4)}, device_id_type=MESH)

    place = lax.broadcasted_iota(jnp.int32, named.shape, 1)
    slot_row = lax.broadcasted_iota(jnp.int32, (LANES, N_SEL * SB), 0)
    slot_col = lax.broadcasted_iota(jnp.int32, (LANES, N_SEL * SB), 1) // SB
    spread = jnp.where(slot_row == slot_col, 1.0, 0.0).astype(BF16)
    for g in range(G):
        named[...] = jnp.full(named.shape, -1, jnp.int32)
        named[:nb, :N_SEL] = ch_ref[:, g, :]
        c = named[...]
        source = jnp.zeros_like(c)
        for s in range(1, n):
            source = source + jnp.where(c >= s * nb, 1, 0)
        inside = c - source * nb
        low_of = jnp.zeros_like(c)
        for s in range(n):
            hit = (c >= 0) & (source == s)
            lo = jnp.where(hit, inside, nb)
            lo = jnp.min(jnp.min(lo, axis=0, keepdims=True), axis=1, keepdims=True)
            lo = jnp.where(lo == nb, 0, lo)
            hi = jnp.where(hit, inside, 0)
            hi = jnp.max(jnp.max(hi, axis=0, keepdims=True), axis=1, keepdims=True)
            low_of = jnp.where(hit, lo, low_of)
            req_ref[s, 2 * g : 2 * g + 1] = jnp.broadcast_to(lo, (1, LANES))
            req_ref[s, 2 * g + 1 : 2 * g + 2] = jnp.broadcast_to(hi, (1, LANES))
        away = G * nb + (source * G + g) * 2 + jnp.where(inside != low_of, 1, 0)
        at = jnp.where(source == me, g * nb + inside, away)
        idx_ref[g] = jnp.where(c >= 0, at, 0)
        again = jnp.zeros(c.shape, F32)
        for d in range(1, N_SEL):
            again = jnp.where((place >= d) & (pltpu.roll(c, d, 1) == c), 1.0, again)
        bias_ref[g] = jnp.dot(again.astype(BF16), spread, preferred_element_type=F32) * LOW

    idx_copy = pltpu.make_async_copy(idx_ref, idx_smem, sem_idx)
    idx_copy.start()
    pl.semaphore_wait(barrier, n + 2)

    def req_copy(i):
        return pltpu.make_async_remote_copy(
            src_ref=req_ref.at[lax.rem(me + n - i, n)], dst_ref=req_in.at[i],
            send_sem=req_s.at[i], recv_sem=req_r.at[i],
            device_id={"kv": lax.rem(me + n - i, n)}, device_id_type=MESH,
        )

    def blk_copy(i):
        return pltpu.make_async_remote_copy(
            src_ref=send.at[i],
            dst_ref=tab_ref.at[pl.ds(G * nb + me * G * 2, G * 2)],
            send_sem=blk_s.at[i], recv_sem=blk_r.at[i],
            device_id={"kv": lax.rem(me + i, n)}, device_id_type=MESH,
        )

    def blk_arrival(i):
        s = lax.rem(me + n - i, n)
        return pltpu.make_async_remote_copy(
            src_ref=send.at[i],
            dst_ref=tab_ref.at[pl.ds(G * nb + s * G * 2, G * 2)],
            send_sem=blk_s.at[i], recv_sem=blk_r.at[i],
            device_id={"kv": lax.rem(me + i, n)}, device_id_type=MESH,
        )

    def sum_copy(i):
        return pltpu.make_async_remote_copy(
            src_ref=sum_send, dst_ref=sum_ref.at[me],
            send_sem=sum_s.at[i], recv_sem=sum_r.at[i],
            device_id={"kv": lax.rem(me + i, n)}, device_id_type=MESH,
        )

    def sum_arrival(i):
        return pltpu.make_async_remote_copy(
            src_ref=sum_send, dst_ref=sum_ref.at[lax.rem(me + n - i, n)],
            send_sem=sum_s.at[i], recv_sem=sum_r.at[i],
            device_id={"kv": lax.rem(me + i, n)}, device_id_type=MESH,
        )

    for i in range(1, n):
        req_copy(i).start()

    acc[:, : 2 * kvd] = jnp.zeros((rows, 2 * kvd), F32)

    def kv_step(i, carry):
        for c in loads(i):
            c.wait()
        acc[:, : 2 * kvd] += jnp.dot(tok[:, part(i)], kvw[part(i), :], preferred_element_type=F32)
        return carry

    lax.fori_loop(0, chunks, kv_step, 0)
    lane = lax.broadcasted_iota(jnp.int32, (SB, LANES), 1)
    lower = lane < HD

    def table_step(b, carry):
        r0 = pl.ds(b * SB, SB)
        for pair in range(G // 2):
            keys = acc[r0, pair * LANES : (pair + 1) * LANES].astype(BF16).astype(F32)
            vals = acc[r0, kvd + pair * LANES : kvd + (pair + 1) * LANES].astype(BF16).astype(F32)
            first = jnp.where(lower, keys, pltpu.roll(vals, HD, 1))
            second = jnp.where(lower, pltpu.roll(keys, HD, 1), vals)
            for g, t in ((2 * pair, first), (2 * pair + 1, second)):
                tf[g * nb + b] = t.astype(BF16)
                tab_ref[g * nb + b] = t.astype(BF16)
        return carry

    lax.fori_loop(0, nb, table_step, 0)
    pos_ref[:, :HD] = pos_in[...].astype(F32)
    pos_ref[:, HD:] = pos_in[...].astype(F32)
    mix_row = lax.broadcasted_iota(jnp.int32, km_ref.shape, 0)
    mix_low = lax.broadcasted_iota(jnp.int32, (CMP, LANES), 1) < HD
    diagonal = lax.broadcasted_iota(jnp.int32, (CMP, CMP), 0) == lax.broadcasted_iota(
        jnp.int32, (CMP, CMP), 1
    )

    def mix_column(ref, head):
        line = jnp.where(mix_row == head, ref[...].astype(F32), 0.0)
        line = jnp.sum(line, axis=0, keepdims=True)
        return jnp.sum(jnp.where(diagonal, line, 0.0), axis=1, keepdims=True)

    for g in range(G):
        head = lax.axis_index("tp") * G + g
        km = mix_column(km_ref, head)
        vm = mix_column(vm_ref, head)
        mix = jnp.where(mix_low, km, vm)
        t = tf[g * nb : (g + 1) * nb].astype(F32).reshape(spans, CMP, LANES)
        w = (t + pos_ref[...][None]) * mix[None]
        s = jnp.sum(w, axis=1)
        s = jnp.concatenate([s, jnp.zeros((pad - spans, LANES), F32)], axis=0)
        sum_send[g] = s.astype(BF16)
        sum_ref[me, g] = s.astype(BF16)
    for i in range(1, n):
        sum_copy(i).start()
    for i in range(1, n):
        req_copy(i).wait_recv()
        pltpu.make_async_copy(req_in.at[i], req_smem.at[i], sem_req.at[i]).start()
    for i in range(1, n):
        pltpu.make_async_copy(req_in.at[i], req_smem.at[i], sem_req.at[i]).wait()

        @pl.when(me + i < n)
        def _():
            for k in range(G * 2):
                send[i, k] = tf[(k // 2) * nb + req_smem[i, k, 0]]
            blk_copy(i).start()

    acc[...] = jnp.zeros_like(acc)
    gacc[...] = jnp.zeros_like(gacc)

    def q_step(i, carry):
        for c in late(i):
            c.wait()
        acc[...] += jnp.dot(tok[:, part(i)], qw[part(i), :], preferred_element_type=F32)
        gacc[...] += lax.dot_general(
            tok[:, part(i)], gw[:, part(i)], (((1,), (1,)), ((), ())), preferred_element_type=F32
        )
        return carry

    lax.fori_loop(0, chunks, q_step, 0)
    gate_ref[...] = jax.nn.sigmoid(gacc[...])

    def query_step(b, carry):
        r0 = pl.ds(b * SB, SB)
        for g in range(G):
            for pair in range(R // 2):
                at = (g * R // 2 + pair) * LANES
                t = acc[r0, at : at + LANES].astype(BF16).astype(F32) * (HD ** -0.5)
                even = jnp.where(lower, t, 0.0)
                odd = jnp.where(lower, pltpu.roll(t, HD, 1), 0.0)
                qp_ref[g, b, 2 * pair * SB : (2 * pair + 1) * SB, :] = even.astype(BF16)
                qp_ref[g, b, (2 * pair + 1) * SB : (2 * pair + 2) * SB, :] = odd.astype(BF16)
        return carry

    lax.fori_loop(0, nb, query_step, 0)
    idx_copy.wait()
    for i in range(1, n):
        sum_arrival(i).wait_recv()
        sum_copy(i).wait_send()
        req_copy(i).wait_send()

        @pl.when(me + i < n)
        def _():
            blk_copy(i).wait_send()

        @pl.when(me - i >= 0)
        def _():
            blk_arrival(i).wait_recv()


def attend_and_mix(
    n, G, R, nb, pad, spans, cw, load,
    idx_ref, qp_ref, gate_ref, tab_ref, sum_ref, bias_ref,
    out_ref,
    ow, att, kbuf, mine, dsend, drecv, early, esend, erecv, xsend, xrecv, base,
    d_s, d_r, e_s, e_r, x_s, x_r,
):
    me = lax.axis_index("kv")
    tp = lax.axis_index("tp")
    core = lax.rem(tp, 2)
    side = tp // 2
    partner = side * 2 + 1 - core
    rows = nb * SB
    quarter = rows // 4
    half_blocks = nb // 2
    width = out_ref.shape[1]
    chunks = width // cw
    group_rows = R * SB
    side_cols = width // 2
    step_rows = SB // 2

    row = lax.broadcasted_iota(jnp.int32, (group_rows, LANES), 0) % SB
    lane = lax.broadcasted_iota(jnp.int32, (group_rows, LANES), 1)
    tri = jnp.where((lane < SB) & (lane > row), LOW, 0.0)
    span_lane = lax.broadcasted_iota(jnp.int32, (group_rows, n * pad), 1)
    span_in = span_lane % pad
    span_end = ((span_lane // pad) * spans + span_in) * CMP + (CMP - 1)
    span_row = lax.broadcasted_iota(jnp.int32, (group_rows, n * pad), 0) % SB
    low64 = lax.broadcasted_iota(jnp.int32, (SB, LANES), 1) < HD
    gate_lane = lax.broadcasted_iota(jnp.int32, (SB, gate_ref.shape[1]), 1)
    nt = (((1,), (1,)), ((), ()))

    def attend(b, carry):
        gates = gate_ref[pl.ds(b * SB, SB), :]
        seen = (span_in < spans) & (span_end - span_row <= me * rows + b * SB)
        for g in range(G):
            for j in range(N_SEL):
                kbuf[g, j * SB : (j + 1) * SB, :] = tab_ref[idx_ref[g, b, j]]
            kb = kbuf[g]
            q = qp_ref[g, b]
            s = lax.dot_general(q, kb, nt, preferred_element_type=F32)
            s = s + bias_ref[g, pl.ds(b, 1), :]
            s = jnp.concatenate([s[:, :LANES] + tri, s[:, LANES:]], axis=1)
            m = jnp.max(s, axis=-1, keepdims=True)
            p = jnp.exp(s - m)
            l = jnp.sum(p, axis=-1, keepdims=True)
            oc = jnp.dot(p.astype(BF16), kb, preferred_element_type=F32)
            sm = sum_ref[:, g].reshape(n * pad, LANES)
            s2 = lax.dot_general(q, sm, nt, preferred_element_type=F32)
            s2 = jnp.where(seen, s2, LOW)
            m2 = jnp.max(s2, axis=-1, keepdims=True)
            p2 = jnp.where(seen, jnp.exp(s2 - m2), 0.0)
            l2 = jnp.sum(p2, axis=-1, keepdims=True)
            os = jnp.dot(p2.astype(BF16), sm, preferred_element_type=F32)
            ic = 1.0 / l
            i2 = jnp.where(l2 > 0.0, 1.0 / jnp.where(l2 > 0.0, l2, 1.0), 0.0)
            parts = []
            for r in range(R):
                at = (tp * G * R + g * R + r) * 2
                g0 = jnp.sum(jnp.where(gate_lane == at, gates, 0.0), axis=-1, keepdims=True)
                g1 = jnp.sum(jnp.where(gate_lane == at + 1, gates, 0.0), axis=-1, keepdims=True)
                k = slice(r * SB, (r + 1) * SB)
                parts.append(os[k] * (g0 * i2[k]) + oc[k] * (g1 * ic[k]))
            for pair in range(R // 2):
                t = jnp.where(low64, pltpu.roll(parts[2 * pair], HD, 1), parts[2 * pair + 1])
                at = (g * R // 2 + pair) * LANES
                att[pl.ds(b * SB, SB), at : at + LANES] = t.astype(BF16)
        return carry

    def d_copy(j):
        return pltpu.make_async_remote_copy(
            src_ref=dsend.at[j], dst_ref=drecv.at[j],
            send_sem=d_s.at[j], recv_sem=d_r.at[j],
            device_id={"tp": partner}, device_id_type=MESH,
        )

    def e_copy(i):
        return pltpu.make_async_remote_copy(
            src_ref=esend.at[i], dst_ref=erecv.at[i],
            send_sem=e_s.at[i], recv_sem=e_r.at[i],
            device_id={"tp": partner}, device_id_type=MESH,
        )

    def x_copy(k):
        step = lax.rem(k, half_blocks)
        return pltpu.make_async_remote_copy(
            src_ref=xsend.at[k], dst_ref=xrecv.at[core, step],
            send_sem=x_s.at[k], recv_sem=x_r.at[core, step],
            device_id={"tp": (1 - side) * 2 + k // half_blocks}, device_id_type=MESH,
        )

    def x_arrival(c, step):
        return pltpu.make_async_remote_copy(
            src_ref=xsend.at[step], dst_ref=xrecv.at[c, step],
            send_sem=x_s.at[step], recv_sem=x_r.at[c, step],
            device_id={"tp": (1 - side) * 2 + core}, device_id_type=MESH,
        )

    other_first = (1 - side) * half_blocks

    def early_block(i):
        attend(other_first + i, 0)
        a = att[pl.ds((other_first + i) * SB, SB), :]
        for j in range(side_cols // cw):
            cols = pl.ds(pl.multiple_of((1 - core) * side_cols + j * cw, cw), cw)
            esend[i, :, j * cw : (j + 1) * cw] = jnp.dot(
                a, ow[:, cols], preferred_element_type=F32
            ).astype(BF16)
        e_copy(i).start()
        for j in range(side_cols // cw):
            cols = pl.ds(pl.multiple_of(core * side_cols + j * cw, cw), cw)
            early[i, :, j * cw : (j + 1) * cw] = jnp.dot(
                a, ow[:, cols], preferred_element_type=F32
            ).astype(BF16)

    def forward(i):
        e_copy(i).wait_recv()
        for k in range(2):
            r = slice(k * step_rows, (k + 1) * step_rows)
            xsend[2 * i + k] = (early[i, r].astype(F32) + erecv[i, r].astype(F32)).astype(BF16)
            x_copy(2 * i + k).start()

    load.wait()

    def early_step(i, carry):
        early_block(i)
        forward(i)
        return carry

    lax.fori_loop(0, half_blocks, early_step, 0)

    own_first = side * half_blocks
    lax.fori_loop(own_first, own_first + half_blocks, attend, 0)

    def own_step(j, carry):
        w = ow[:, pl.ds(pl.multiple_of(j * cw, cw), cw)]
        theirs = att[pl.ds(own_first * SB + (1 - core) * quarter, quarter), :]
        dsend[j] = jnp.dot(theirs, w, preferred_element_type=F32).astype(BF16)
        d_copy(j).start()
        ours = att[pl.ds(own_first * SB + core * quarter, quarter), :]
        mine[j] = jnp.dot(ours, w, preferred_element_type=F32).astype(BF16)
        return carry

    lax.fori_loop(0, chunks, own_step, 0)

    def base_step(j, carry):
        d_copy(j).wait_recv()
        cols = pl.ds(pl.multiple_of(j * cw, cw), cw)
        base[:, cols] = mine[j].astype(F32) + drecv[j].astype(F32)
        d_copy(j).wait_send()
        return carry

    lax.fori_loop(0, chunks, base_step, 0)

    def last_step(k, carry):
        r = pl.ds(pl.multiple_of(k * step_rows, step_rows), step_rows)
        for c in range(2):
            x_arrival(c, k).wait_recv()
            cols = slice(c * side_cols, (c + 1) * side_cols)
            out_ref[r, cols] = (base[r, cols] + xrecv[c, k].astype(F32)).astype(BF16)
        e_copy(k).wait_send()
        x_copy(k).wait_send()
        x_copy(half_blocks + k).wait_send()
        return carry

    lax.fori_loop(0, half_blocks, last_step, 0)


def layer_kernel(n, G, R, nb, kc, pad, cw, *refs):
    inputs, ow_hbm, out_ref = refs[:9], refs[9], refs[10]
    qp, gate, tab, summary, idx, bias = refs[11:17]
    idx_smem, sem_idx, ow, sem_w = refs[17:21]
    first, second = refs[21 : 21 + 26], refs[21 + 26 :]
    load = pltpu.make_async_copy(ow_hbm, ow, sem_w)
    project(
        n, G, R, nb, kc, pad, load, idx_smem, sem_idx,
        *inputs, qp, gate, tab, summary, idx, bias, *first,
    )
    attend_and_mix(
        n, G, R, nb, pad, nb * SB // CMP, cw, load,
        idx_smem, qp, gate, tab, summary, bias, out_ref, ow, *second,
    )


def local(
    n,
    tokens, query_weight, key_weight, value_weight, gate_weight,
    summary_pos, key_mixing, value_mixing, out_weight, chosen,
):
    rows, depth = tokens.shape
    heads = query_weight.shape[1] // HD
    G = key_weight.shape[1] // HD
    R = heads // G
    nb = rows // SB
    spans = rows // CMP
    pad = -(-spans // 16) * 16
    kc = min(1024, depth)
    chunks = depth // kc
    width = out_weight.shape[1]
    cw = 512
    oc = width // cw
    gates_all = gate_weight.shape[1]

    vmem = pl.BlockSpec(memory_space=pltpu.VMEM)
    hbm = pl.BlockSpec(memory_space=pl.ANY)
    dma = pltpu.SemaphoreType.DMA
    table = G * nb + n * G * 2
    nbp = -(-nb // 8) * 8
    quarter = rows // 4
    half = nb // 2
    stage_one = [
        pltpu.VMEM((rows, depth), BF16),
        pltpu.VMEM((depth, heads * HD), BF16),
        pltpu.VMEM((depth, 2 * G * HD), BF16),
        pltpu.VMEM((gates_all, depth), BF16),
        pltpu.VMEM((rows, heads * HD), F32),
        pltpu.VMEM((rows, gates_all), F32),
        pltpu.VMEM((G * nb, SB, LANES), BF16),
        pltpu.VMEM((nbp, LANES), jnp.int32),
        pltpu.VMEM((CMP, LANES), F32),
        pltpu.VMEM((n, 8, LANES), jnp.int32),
        pltpu.VMEM((n, 8, LANES), jnp.int32),
        pltpu.SMEM((n, 8, LANES), jnp.int32),
        dma((n,)),
        pltpu.VMEM((n, G * 2, SB, LANES), BF16),
        pltpu.VMEM((G, pad, LANES), BF16),
        dma((chunks,)), dma((chunks,)), dma((chunks,)), dma((chunks,)), dma((chunks,)),
        dma((n,)), dma((n,)), dma((n,)), dma((n,)), dma((n,)), dma((n,)),
    ]
    stage_two = [
        pltpu.VMEM((rows, heads * HD), BF16),
        pltpu.VMEM((G, N_SEL * SB, LANES), BF16),
        pltpu.VMEM((oc, quarter, cw), BF16),
        pltpu.VMEM((oc, quarter, cw), BF16),
        pltpu.VMEM((oc, quarter, cw), BF16),
        pltpu.VMEM((half, SB, width // 2), BF16),
        pltpu.VMEM((half, SB, width // 2), BF16),
        pltpu.VMEM((half, SB, width // 2), BF16),
        pltpu.VMEM((2 * half, SB // 2, width // 2), BF16),
        pltpu.VMEM((2, half, SB // 2, width // 2), BF16),
        pltpu.VMEM((quarter, width), F32),
        dma((oc,)), dma((oc,)), dma((half,)), dma((half,)), dma((2 * half,)), dma((2, half)),
    ]
    return pl.pallas_call(
        functools.partial(layer_kernel, n, G, R, nb, kc, pad, cw),
        name="layer",
        out_shape=jax.ShapeDtypeStruct((quarter, width), BF16),
        in_specs=[hbm] * 5 + [vmem] * 4 + [hbm],
        out_specs=vmem,
        scratch_shapes=[
            pltpu.VMEM((G, nb, R * SB, LANES), BF16),
            pltpu.VMEM((rows, gates_all), F32),
            pltpu.VMEM((table, SB, LANES), BF16),
            pltpu.VMEM((n, G, pad, LANES), BF16),
            pltpu.VMEM((G, nbp, LANES), jnp.int32),
            pltpu.VMEM((G, nbp, N_SEL * SB), F32),
            pltpu.SMEM((G, nbp, LANES), jnp.int32),
            dma,
            pltpu.VMEM(out_weight.shape, BF16),
            dma,
            *stage_one,
            *stage_two,
        ],
        compiler_params=pltpu.CompilerParams(
            collective_id=1, has_side_effects=True, vmem_limit_bytes=VMEM_LIMIT
        ),
    )(
        tokens, query_weight, key_weight, value_weight, gate_weight.T,
        chosen, key_mixing.T, value_mixing.T, summary_pos, out_weight,
    )


def solution(mesh):
    placed = (
        P("kv", None),
        P(None, "tp"),
        P(None, "tp"),
        P(None, "tp"),
        P(),
        P(),
        P(),
        P(),
        P("tp", None),
        P("kv", "tp", None),
    )
    return jax.shard_map(
        functools.partial(local, mesh.shape["kv"]),
        mesh=mesh, in_specs=placed, out_specs=P(("kv", "tp"), None), check_vma=False,
    )
```
